32 devices in a mesh: sp: 16 (over z, y, x), tp: 2 (over core).
Axes of the slice: x: 2, y: 2, z: 4, core: 2. Of those that a mesh axis runs over, the one named last changes fastest.
Arguments:
- tokens: bfloat16 [8192, 2048], P('sp', 'tp'), may hold values from -6 to 6
- norm_gain: float32 [2048], replicated, may hold values from 0.1 to 1.9
- outer_gate: bfloat16 [2048, 1024], P('sp', 'tp'), may hold values from -0.125 to 0.125
- inner_gate: bfloat16 [2048, 1024], P('sp', 'tp'), may hold values from -0.125 to 0.125
- conv_input: bfloat16 [2048, 1024], P('sp', 'tp'), may hold values from -0.125 to 0.125
- query_proj: bfloat16 [2048, 1024], P('sp', 'tp'), may hold values from -0.125 to 0.125
- key_proj: bfloat16 [2048, 1024], P('sp', 'tp'), may hold values from -0.125 to 0.125
- value_proj: bfloat16 [2048, 1024], P('sp', 'tp'), may hold values from -0.125 to 0.125
- out_gate: bfloat16 [2048, 1024], P('sp', 'tp'), may hold values from -0.125 to 0.125
- conv_taps: float32 [3, 1024], P(None, 'tp'), may hold values from -3.5 to 3.5
- log_decay: float32 [2, 16, 8192], P(None, 'tp', 'sp'), may hold values from -1.2 to 0, as said below
- head_gain: float32 [1024], P('tp'), may hold values from 0.1 to 1.9
- conv_output: bfloat16 [1024, 2048], P('tp', 'sp'), may hold values from -0.1875 to 0.1875
- retention_output: bfloat16 [1024, 2048], P('tp', 'sp'), may hold values from -0.1875 to 0.1875
Outputs:
- mixed: bfloat16 [8192, 2048], P(('sp', 'tp'))
The draws below stay inside these ranges and needn't reach their ends.
Inputs may be any that keep to these rules, and one draw needn't show every extreme that they name: `log_decay`: logarithms of per-position decays, below zero.
All inputs are finite; a program needn't handle non-finite values.
Results may differ from the reference program's by a relative error of at most 0.02.
Values may be sent and summed in bfloat16 or wider, within the bound.
No kernel may reach another device: no remote copies, remote signals or barrier semaphores. Data moves between devices by JAX's collectives and lax.ppermute only.
A program may use at most 128 MiB of HBM per device.

```python
import math
import jax
import jax.numpy as jnp
from jax import lax

D = 2048
CONV_CH = 1024
HEAD_NUMBER = 16
HEAD_DIM = 64
TOK_DEV = 512
TOKEN_NUMBER = 8192
N_SP = 16
N_TP = 2


def draw_log_decay(key, part):
    key_sequence = jax.random.split(jax.random.fold_in(key, 17), 6)
    span_count = TOKEN_NUMBER // TOK_DEV
    is_fast = jax.random.uniform(key_sequence[0], (2, HEAD_NUMBER, 1), jnp.float32) < 0.5
    fast_rate = jax.random.uniform(key_sequence[1], (2, HEAD_NUMBER, 1), jnp.float32, 0.01, 0.02)
    slow_rate = jax.random.uniform(key_sequence[2], (2, HEAD_NUMBER, 1), jnp.float32, 0.1, 0.3) / TOKEN_NUMBER
    selected_rate = jnp.where(is_fast, fast_rate, slow_rate)
    multiplier = jnp.exp(jax.random.uniform(key_sequence[3], (2, HEAD_NUMBER, span_count), jnp.float32, 0.0, math.log(4.0)))
    multiplier = jnp.repeat(multiplier, TOK_DEV, axis=2)
    flurry_location = jax.random.randint(key_sequence[4], (2, HEAD_NUMBER, 2, 1), 0, TOKEN_NUMBER)
    flurry_depth = jax.random.uniform(key_sequence[5], (2, HEAD_NUMBER, 2, 1), jnp.float32, 0.22, 0.51)
    position_list = jnp.arange(TOKEN_NUMBER, dtype=jnp.int32)
    flurry_list = jnp.sum(jnp.where(position_list == flurry_location, flurry_depth, 0.0), axis=2)
    return (-(selected_rate * multiplier) - flurry_list).astype(jnp.float32)


def shard_levels(stream_key, dims, pieces, least, largest):
    gain, own = 1.0, jax.random.fold_in(stream_key, 6)
    for axis_at, blocks in pieces:
        steps = jnp.exp(jax.random.uniform(jax.random.fold_in(own, axis_at), (blocks,), jnp.float32, least / len(pieces), largest / len(pieces)))
        gain = gain * jnp.repeat(steps, dims[axis_at] // blocks).reshape([-1 if axis == axis_at else 1 for axis in range(len(dims))])
    return gain


def centred(stream_key, dims, width, reach, cuts=(), held_as=jnp.bfloat16):
    gain = shard_levels(stream_key, dims, cuts, -0.22, 0.18) if cuts else 1.0
    entries = jax.random.normal(stream_key, dims, jnp.float32) * width * gain
    return jnp.minimum(jnp.maximum(entries, -reach), reach).astype(held_as)


def setup_inputs(seed: int = 0) -> dict:
    seeds = jax.random.split(jax.random.key(seed), 15)
    tokens = centred(seeds[0], (TOKEN_NUMBER, D), 1.0, 6.0, ((0, 16), (1, 2)))
    norm_gain = jnp.clip(1.0 + 0.18 * jax.random.normal(seeds[1], (D,), jnp.float32), 0.1, 1.9)
    outer_gate = centred(seeds[2], (D, CONV_CH), D ** -0.5, 0.125, ((0, 16), (1, 2)))
    inner_gate = centred(seeds[3], (D, CONV_CH), D ** -0.5, 0.125, ((0, 16), (1, 2)))
    conv_input = centred(seeds[4], (D, CONV_CH), D ** -0.5, 0.125, ((0, 16), (1, 2)))
    query_proj = centred(seeds[5], (D, HEAD_NUMBER * HEAD_DIM), D ** -0.5, 0.125, ((0, 16), (1, 2)))
    key_proj = centred(seeds[6], (D, HEAD_NUMBER * HEAD_DIM), D ** -0.5, 0.125, ((0, 16), (1, 2)))
    value_proj = centred(seeds[7], (D, HEAD_NUMBER * HEAD_DIM), D ** -0.5, 0.125, ((0, 16), (1, 2)))
    out_gate = centred(seeds[8], (D, HEAD_NUMBER * HEAD_DIM), D ** -0.5, 0.125, ((0, 16), (1, 2)))
    conv_taps = centred(seeds[9], (3, CONV_CH), 3 ** -0.5, 3.5, ((1, 2),), jnp.float32)
    log_decay = draw_log_decay(jax.random.fold_in(seeds[14], 71), 0)
    head_gain = jnp.clip(1.0 + 0.18 * jax.random.normal(seeds[11], (HEAD_NUMBER * HEAD_DIM,), jnp.float32), 0.1, 1.9)
    conv_output = centred(seeds[12], (CONV_CH, D), CONV_CH ** -0.5, 0.1875, ((0, 2), (1, 16)))
    retention_output = centred(seeds[13], (HEAD_NUMBER * HEAD_DIM, D), (HEAD_NUMBER * HEAD_DIM) ** -0.5, 0.1875, ((0, 2), (1, 16)))
    return {"tokens": tokens, "norm_gain": norm_gain, "outer_gate": outer_gate, "inner_gate": inner_gate, "conv_input": conv_input, "query_proj": query_proj, "key_proj": key_proj, "value_proj": value_proj, "out_gate": out_gate, "conv_taps": conv_taps, "log_decay": log_decay, "head_gain": head_gain, "conv_output": conv_output, "retention_output": retention_output}


EPS = 1e-06
THETA = 10000.0

def rounded(array):
    return lax.optimization_barrier(array.astype(jnp.bfloat16)).astype(jnp.float32)

def rotate(field_in, position_list):
    half_dim = field_in.shape[-1] // 2
    frequency = jnp.exp(-jnp.log(THETA) * jnp.arange(half_dim, dtype=jnp.float32) * (2.0 / field_in.shape[-1]))
    angles = position_list.astype(jnp.float32)[:, None, None] * frequency
    cosine = jnp.cos(angles)
    sine_part = jnp.sin(angles)
    leading = field_in[..., :half_dim]
    trailing = field_in[..., half_dim:]
    return jnp.concatenate([leading * cosine - trailing * sine_part, leading * sine_part + trailing * cosine], axis=-1)

def span_parts(query_rows, key_rows, value_rows, log_rates):
    length = query_rows.shape[0]
    forward_cum = jnp.cumsum(log_rates[0], axis=-1)
    backward_cum = jnp.flip(jnp.cumsum(jnp.flip(log_rates[1], -1), axis=-1), -1)
    row_index = lax.broadcasted_iota(jnp.int32, (length, length), 0)
    col_index = lax.broadcasted_iota(jnp.int32, (length, length), 1)
    lower_part = (col_index <= row_index)[None]
    spread = jnp.where(lower_part, forward_cum[:, :, None] - forward_cum[:, None, :], backward_cum[:, :, None] - backward_cum[:, None, :])
    scores = jnp.einsum('ihe,jhe->hij', query_rows.astype(jnp.float32), key_rows.astype(jnp.float32))
    weighted = rounded(scores * jnp.exp(spread))
    local_part = jnp.einsum('hij,jhe->ihe', weighted, value_rows.astype(jnp.float32))
    key_wide = key_rows.astype(jnp.float32)
    forward_keys = rounded(key_wide * jnp.exp(forward_cum[:, -1:] - forward_cum).T[:, :, None])
    backward_keys = rounded(key_wide * jnp.exp(backward_cum[:, :1] - backward_cum).T[:, :, None])
    forward_state = jnp.einsum('jhd,jhe->hde', forward_keys, value_rows.astype(jnp.float32))
    backward_state = jnp.einsum('jhd,jhe->hde', backward_keys, value_rows.astype(jnp.float32))
    return (local_part, forward_cum, backward_cum, forward_state, backward_state)

def span_item(inputs):
    return span_parts(inputs[0], inputs[1], inputs[2], inputs[3])

def carried(query_rows, forward_cum, backward_cum, into_forward, into_backward):
    query_wide = query_rows.astype(jnp.float32)
    forward_part = jnp.einsum('ihd,hde->ihe', query_wide, rounded(into_forward))
    backward_part = jnp.einsum('ihd,hde->ihe', query_wide, rounded(into_backward))
    return jnp.exp(forward_cum).T[:, :, None] * forward_part + jnp.exp(backward_cum).T[:, :, None] * backward_part

def finish(mixed_heads, gate_rows, head_gain):
    row_count, head_count, head_width = mixed_heads.shape
    scaled = mixed_heads * lax.rsqrt(lax.optimization_barrier(jnp.mean(mixed_heads * mixed_heads, axis=-1, keepdims=True)) + EPS)
    scaled = scaled * head_gain.reshape(head_count, head_width)
    return (jax.nn.silu(gate_rows.astype(jnp.float32)) * scaled.reshape(row_count, head_count * head_width)).astype(jnp.bfloat16)

def forward_step(running, inputs):
    return (jnp.exp(inputs[0])[:, None, None] * running + inputs[1], running)

def reference(tokens, norm_gain, outer_gate, inner_gate, conv_input, query_proj, key_proj, value_proj, out_gate, conv_taps, log_decay, head_gain, conv_output, retention_output):
    wide = tokens.astype(jnp.float32)
    normed = (wide * lax.rsqrt(lax.optimization_barrier(jnp.mean(wide * wide, axis=-1, keepdims=True)) + EPS) * norm_gain).astype(jnp.bfloat16)
    projected = [jnp.dot(normed, weight, preferred_element_type=jnp.float32).astype(jnp.bfloat16) for weight in (outer_gate, inner_gate, conv_input, query_proj, key_proj, value_proj, out_gate)]
    inner_value = (projected[1].astype(jnp.float32) * projected[2].astype(jnp.float32)).astype(jnp.bfloat16)
    padded = jnp.pad(inner_value.astype(jnp.float32), ((1, 1), (0, 0)))
    convolved = conv_taps[0] * padded[:-2] + conv_taps[1] * padded[1:-1] + conv_taps[2] * padded[2:]
    conv_out = (projected[0].astype(jnp.float32) * convolved).astype(jnp.bfloat16)
    position_list = jnp.arange(TOKEN_NUMBER, dtype=jnp.int32)
    shape_heads = (TOKEN_NUMBER, HEAD_NUMBER, HEAD_DIM)
    rotated_query = rotate(projected[3].astype(jnp.float32).reshape(shape_heads), position_list).astype(jnp.bfloat16)
    rotated_key = (rotate(projected[4].astype(jnp.float32).reshape(shape_heads), position_list) * HEAD_DIM ** (-0.5)).astype(jnp.bfloat16)
    value_heads = projected[5].reshape(shape_heads)
    span_shape = (N_SP, TOK_DEV, HEAD_NUMBER, HEAD_DIM)
    span_rates = log_decay.reshape(2, HEAD_NUMBER, N_SP, TOK_DEV).transpose(2, 0, 1, 3)
    span_query = rotated_query.reshape(span_shape)
    local_part, forward_cum, backward_cum, forward_state, backward_state = lax.map(span_item, (span_query, rotated_key.reshape(span_shape), value_heads.reshape(span_shape), span_rates))
    blank = jnp.zeros((HEAD_NUMBER, HEAD_DIM, HEAD_DIM), jnp.float32)
    into_forward = lax.scan(forward_step, blank, (forward_cum[:, :, -1], forward_state))[1]
    into_backward = lax.scan(forward_step, blank, (backward_cum[:, :, 0], backward_state), reverse=True)[1]
    carried_part = jax.vmap(carried)(span_query, forward_cum, backward_cum, into_forward, into_backward)
    mixed_heads = (local_part + carried_part).reshape(shape_heads)
    ret_out = finish(mixed_heads, projected[6], head_gain)
    conv_group = CONV_CH // N_TP
    ret_group = HEAD_NUMBER * HEAD_DIM // N_TP
    total_sum = jnp.zeros((TOKEN_NUMBER, D), jnp.float32)
    for group_index in range(N_TP):
        conv_lo = group_index * conv_group
        ret_lo = group_index * ret_group
        partial_sum = jnp.dot(conv_out[:, conv_lo:conv_lo + conv_group], conv_output[conv_lo:conv_lo + conv_group], preferred_element_type=jnp.float32)
        partial_sum = partial_sum + jnp.dot(ret_out[:, ret_lo:ret_lo + ret_group], retention_output[ret_lo:ret_lo + ret_group], preferred_element_type=jnp.float32)
        total_sum = total_sum + rounded(partial_sum)
    return total_sum.astype(jnp.bfloat16)
```

```python
import jax
import jax.numpy as jnp
from jax import lax
from jax.sharding import PartitionSpec as P

HEAD_DIM = 64
EPS = 1e-06
THETA = 10000.0


F32 = jnp.float32
BF16 = jnp.bfloat16


def sequence_dims(mesh):
    total = mesh.shape["sp"]
    column = mesh.devices[:, 0]
    places = [getattr(d, "coords", None) for d in column]
    if any(place is None for place in places):
        return (total,)
    sizes, product = [], 1
    for axis in (2, 1, 0):
        count = len({place[axis] for place in places})
        if count > 1:
            sizes.append(count)
            product *= count
    if product != total:
        return (total,)
    return tuple(sizes)


def make_local(dims, n_tp):
    n_sp = 1
    for size in dims:
        n_sp *= size
    pair = 2 if len(dims) > 1 and dims[-1] == 2 else 1
    outer = dims[:-1] if pair == 2 else dims
    n_unit = n_sp // pair
    strides = []
    left = n_unit
    for size in outer:
        left //= size
        strides.append(left)

    def shifted(axis, step):
        size, stride = outer[axis], strides[axis]
        moves = []
        for i in range(n_sp):
            unit, lane = divmod(i, pair)
            at = (unit // stride) % size
            to = unit + ((at + step) % size - at) * stride
            moves.append((i, to * pair + lane))
        return moves

    def send(x, axis, step):
        return lax.ppermute(x, "sp", shifted(axis, step))

    def gather_units(block):
        held = block[None]
        for axis, size in enumerate(outer):
            parts = [held] + [send(held, axis, step) for step in range(1, size)]
            held = jnp.concatenate(parts, axis=0)
        return held

    def relative_units(unit):
        order = [unit]
        for axis, size in enumerate(outer):
            stride = strides[axis]
            grown = []
            for step in range(size):
                for u in order:
                    at = (u // stride) % size
                    grown.append(u + ((at - step + size) % size - at) * stride)
            order = grown
        return order

    def relative_place(unit, other):
        place, scale = 0, 1
        for axis, size in enumerate(outer):
            stride = strides[axis]
            gap = ((unit // stride) % size - (other // stride) % size + size) % size
            place = place + gap * scale
            scale *= size
        return place

    def swap_pair(x):
        return lax.ppermute(x, "sp", [(i, i ^ 1) for i in range(n_sp)])

    def swap_tp(x):
        return lax.ppermute(x, "tp", [(0, 1), (1, 0)])

    def in_order(first, mine, other, axis):
        a = jnp.where(first == 0, mine, other)
        b = jnp.where(first == 0, other, mine)
        return jnp.concatenate([a, b], axis=axis)

    def exchange_columns(block, lane, axis):
        if pair == 1:
            return block
        half = block.shape[axis] // 2
        mine = lax.dynamic_slice_in_dim(block, lane * half, half, axis)
        theirs = lax.dynamic_slice_in_dim(block, (1 - lane) * half, half, axis)
        return mine, swap_pair(theirs)

    def local(
        tokens, norm_gain, outer_gate, inner_gate, conv_input, query_proj, key_proj,
        value_proj, out_gate, conv_taps, log_decay, head_gain, conv_output, retention_output,
    ):
        own = lax.axis_index("sp")
        unit, lane = own // pair, own % pair
        tp = lax.axis_index("tp")
        span = tokens.shape[0]
        rows = span * pair
        width = outer_gate.shape[1] // pair
        heads = width // HEAD_DIM
        kdepth = outer_gate.shape[0]

        def half(x, axis):
            return lax.dynamic_slice_in_dim(x, lane * (x.shape[axis] // pair), x.shape[axis] // pair, axis)

        def in_chunk(*weights):
            if pair == 1:
                return gather_units(jnp.concatenate(weights, axis=1))
            size = weights[0].shape[1] // 2
            mine = jnp.concatenate([lax.dynamic_slice_in_dim(w, lane * size, size, 1) for w in weights], axis=1)
            theirs = jnp.concatenate(
                [lax.dynamic_slice_in_dim(w, (1 - lane) * size, size, 1) for w in weights], axis=1
            )
            return gather_units(in_order(lane, mine, swap_pair(theirs), 0))

        def out_chunk(*weights):
            if pair == 1:
                return gather_units(jnp.concatenate(weights, axis=0))
            size = weights[0].shape[0] // 2
            mine = jnp.concatenate([lax.dynamic_slice_in_dim(w, lane * size, size, 0) for w in weights], axis=0)
            theirs = jnp.concatenate(
                [lax.dynamic_slice_in_dim(w, (1 - lane) * size, size, 0) for w in weights], axis=0
            )
            return gather_units(in_order(lane, mine, swap_pair(theirs), 1))

        weights_kv = in_chunk(key_proj, value_proj)
        if pair == 2:
            both = in_order(lane, tokens, swap_pair(tokens), 0)
        else:
            both = tokens
        if n_tp == 2:
            whole = in_order(tp, both, swap_tp(both), 1)
        else:
            whole = lax.all_gather(both, "tp", axis=1, tiled=True)
        if pair == 2:
            rates_theirs = lax.dynamic_slice_in_dim(log_decay, (1 - lane) * heads, heads, 1)
            rates = in_order(lane, half(log_decay, 1), swap_pair(rates_theirs), 2)
        else:
            rates = log_decay
        weights_qg = in_chunk(query_proj, out_gate)
        weights_conv = in_chunk(inner_gate, conv_input, outer_gate)
        weights_out = out_chunk(conv_output, retention_output)

        wide = whole.astype(F32)
        normed = (
            wide * lax.rsqrt(jnp.mean(wide * wide, axis=-1, keepdims=True) + EPS) * norm_gain
        ).astype(BF16)
        order = relative_units(unit)
        piece = kdepth * pair
        normed = jnp.concatenate(
            [lax.dynamic_slice_in_dim(normed, u * piece, piece, 1) for u in order], axis=1
        )

        rates = rates.reshape(2, heads, pair, span)
        cf = jnp.cumsum(rates[0], axis=-1)
        rb = jnp.flip(jnp.cumsum(jnp.flip(rates[1], -1), axis=-1), -1)
        cf_rows = cf.transpose(1, 2, 0)
        rb_rows = rb.transpose(1, 2, 0)

        half_dim = HEAD_DIM // 2
        positions = (unit * rows + lax.iota(jnp.int32, rows)).astype(F32)
        frequency = jnp.exp(-jnp.log(THETA) * jnp.arange(half_dim, dtype=F32) * (2.0 / HEAD_DIM))
        angles = positions[:, None] * frequency
        cosine, sine = lax.optimization_barrier((jnp.cos(angles), jnp.sin(angles)))

        def rotate(x):
            x = x.astype(F32).reshape(rows, heads, HEAD_DIM)
            a, b = x[..., :half_dim], x[..., half_dim:]
            c, s = cosine[:, None], sine[:, None]
            return jnp.concatenate([a * c - b * s, a * s + b * c], axis=-1)

        def project(weights):
            flat = weights.reshape(-1, weights.shape[-1])
            return jnp.dot(normed, flat, preferred_element_type=F32).astype(BF16)

        kv = project(weights_kv)
        by_span = (pair, span, heads, HEAD_DIM)
        key = (rotate(kv[:, :width]) * HEAD_DIM ** (-0.5)).astype(BF16).reshape(by_span)
        value = kv[:, width:].reshape(by_span)
        key_wide = key.astype(F32)
        total_f, total_b = cf[:, :, -1], rb[:, :, 0]
        kf = (key_wide * jnp.exp(cf_rows[:, -1:] - cf_rows)[..., None]).astype(BF16)
        kb = (key_wide * jnp.exp(rb_rows[:, :1] - rb_rows)[..., None]).astype(BF16)
        state_f = jnp.einsum("sjhd,sjhe->shde", kf, value, preferred_element_type=F32)
        state_b = jnp.einsum("sjhd,sjhe->shde", kb, value, preferred_element_type=F32)

        unit_f, unit_b = state_f[0], state_b[pair - 1]
        for s in range(1, pair):
            unit_f = jnp.exp(total_f[:, s])[:, None, None] * unit_f + state_f[s]
            r = pair - 1 - s
            unit_b = jnp.exp(total_b[:, r])[:, None, None] * unit_b + state_b[r]
        unit_total = jnp.stack([total_f.sum(1), total_b.sum(1)])
        packed = jnp.concatenate(
            [
                jnp.stack([unit_f, unit_b]).reshape(2 * heads, HEAD_DIM * HEAD_DIM),
                jnp.broadcast_to(unit_total.reshape(2 * heads, 1), (2 * heads, 128)),
            ],
            axis=1,
        )
        pieces = gather_units(packed)
        states = pieces[:, :, : HEAD_DIM * HEAD_DIM].reshape(n_unit, 2, heads, HEAD_DIM, HEAD_DIM)
        totals = pieces[:, :, HEAD_DIM * HEAD_DIM].reshape(n_unit, 2, heads)
        ids = jnp.stack(order)
        before = (ids[None, :] < ids[:, None]) & (ids[:, None] < unit)
        after = (ids[None, :] > ids[:, None]) & (ids[:, None] > unit)
        gap_f = jnp.sum(
            jnp.where(((ids[None, :] > ids[:, None]) & (ids[None, :] < unit))[..., None], totals[None, :, 0], 0.0), axis=1
        )
        gap_b = jnp.sum(
            jnp.where(((ids[None, :] < ids[:, None]) & (ids[None, :] > unit))[..., None], totals[None, :, 1], 0.0), axis=1
        )
        weight_f = jnp.where((ids < unit)[:, None], jnp.exp(gap_f), 0.0)
        weight_b = jnp.where((ids > unit)[:, None], jnp.exp(gap_b), 0.0)
        into_f = [jnp.sum(weight_f[..., None, None] * states[:, 0], axis=0)]
        into_b = [jnp.sum(weight_b[..., None, None] * states[:, 1], axis=0)]
        for s in range(1, pair):
            into_f.append(jnp.exp(total_f[:, s - 1])[:, None, None] * into_f[-1] + state_f[s - 1])
            r = pair - s
            into_b.append(jnp.exp(total_b[:, r])[:, None, None] * into_b[-1] + state_b[r])
        into_f = jnp.stack(into_f).astype(BF16)
        into_b = jnp.stack(into_b[::-1]).astype(BF16)

        qg = project(weights_qg)
        query = rotate(qg[:, :width]).astype(BF16).reshape(by_span)
        gate = qg[:, width:]
        i_at = lax.broadcasted_iota(jnp.int32, (span, span), 0)
        j_at = lax.broadcasted_iota(jnp.int32, (span, span), 1)
        cfs, rbs = cf.transpose(1, 0, 2), rb.transpose(1, 0, 2)
        spread = jnp.where(
            j_at <= i_at, cfs[..., :, None] - cfs[..., None, :], rbs[..., :, None] - rbs[..., None, :]
        )
        scores = jnp.einsum("sihe,sjhe->shij", query, key, preferred_element_type=F32)
        probs = (scores * jnp.exp(spread)).astype(BF16)
        mix = jnp.einsum("shij,sjhe->sihe", probs, value, preferred_element_type=F32)
        part_f = jnp.einsum("sihd,shde->sihe", query, into_f, preferred_element_type=F32)
        part_b = jnp.einsum("sihd,shde->sihe", query, into_b, preferred_element_type=F32)
        mix = mix + jnp.exp(cf_rows)[..., None] * part_f + jnp.exp(rb_rows)[..., None] * part_b
        scaled = mix * lax.rsqrt(jnp.mean(mix * mix, axis=-1, keepdims=True) + EPS)
        scaled = scaled * half(head_gain, 0).reshape(heads, HEAD_DIM)
        ret_out = (jax.nn.silu(gate.astype(F32)) * scaled.reshape(rows, width)).astype(BF16)

        conv = project(weights_conv)
        inner = (conv[:, :width].astype(F32) * conv[:, width : 2 * width].astype(F32)).astype(BF16)
        ups = [(i, i + pair) for i in range(n_sp - pair)]
        downs = [(i + pair, i) for i in range(n_sp - pair)]
        prior = lax.ppermute(inner[-1:], "sp", ups)
        later = lax.ppermute(inner[:1], "sp", downs)
        padded = jnp.concatenate([prior, inner, later], axis=0).astype(F32)
        taps = half(conv_taps, 1)
        convolved = taps[0] * padded[:-2] + taps[1] * padded[1:-1] + taps[2] * padded[2:]
        conv_out = (conv[:, 2 * width :].astype(F32) * convolved).astype(BF16)

        mixed_in = jnp.concatenate([conv_out, ret_out], axis=1)

        def partial(at):
            x = lax.dynamic_slice_in_dim(mixed_in, at * span, span, 0)
            y = jnp.einsum("pk,bkn->pbn", x, weights_out, preferred_element_type=F32)
            return y.astype(BF16).reshape(span, -1)

        share = span // n_tp

        def over_tp(y):
            if n_tp != 2:
                return lax.psum_scatter(y, "tp", scatter_dimension=0, tiled=True)
            keep = lax.dynamic_slice_in_dim(y, tp * share, share, 0)
            give = lax.dynamic_slice_in_dim(y, (1 - tp) * share, share, 0)
            return (keep.astype(F32) + swap_tp(give).astype(F32)).astype(BF16)

        if pair == 2:
            given = swap_pair(over_tp(partial(1 - lane)))
            total = (over_tp(partial(lane)).astype(F32) + given.astype(F32)).astype(BF16)
        else:
            total = over_tp(partial(0))
        wide_piece = total.shape[1] // n_unit
        return jnp.concatenate(
            [
                lax.dynamic_slice_in_dim(total, relative_place(unit, u) * wide_piece, wide_piece, 1)
                for u in range(n_unit)
            ],
            axis=1,
        )

    return local


def solution(mesh):
    return jax.shard_map(
        make_local(sequence_dims(mesh), mesh.shape["tp"]),
        mesh=mesh,
        in_specs=(
            P("sp", "tp"),
            P(),
            P("sp", "tp"),
            P("sp", "tp"),
            P("sp", "tp"),
            P("sp", "tp"),
            P("sp", "tp"),
            P("sp", "tp"),
            P("sp", "tp"),
            P(None, "tp"),
            P(None, "tp", "sp"),
            P("tp"),
            P("tp", "sp"),
            P("tp", "sp"),
        ),
        out_specs=P(("sp", "tp"), None),
        check_vma=False,
    )
```
